32 devices in a mesh: sp: 16 (over z, x, core), tp: 2 (over y).
Axes of the slice: x: 2, y: 2, z: 4, core: 2. Of those that a mesh axis runs over, the one named last changes fastest.
Arguments:
- skip_connection_stream: bfloat16 [12288, 2048], P('sp'), may hold values from -6 to 6
- probing_vectors: bfloat16 [12288, 512], P('sp', 'tp'), may hold values from -6 to 6
- addressing_vectors: bfloat16 [12288, 512], P('sp', 'tp'), may hold values from -6 to 6
- mapped_payloads: bfloat16 [12288, 1024], P('sp', 'tp'), may hold values from -6 to 6
- emission_switch: bfloat16 [12288, 1024], P('sp', 'tp'), may hold values from -6 to 6
- lapse_preactivation: bfloat16 [12288, 512], P('sp', 'tp')
- lapse_shift_entries: float32 [512], P('tp')
- surplus_attenuation_terms: float32 [12288], P('sp'), may hold values from -0.7 to 0
- passage_label_per_token: int32 [12288], P('sp'), may hold values from 0 to 3, never falling along the last dimension, each value on 1 to 6144 neighbouring positions
- attention_group_rescaler: float32 [128], replicated, may hold values from 0.1 to 1.9
- emission_projector: bfloat16 [1024, 2048], P('tp'), may hold values from -0.1875 to 0.1875
- perceptron_rescaler: float32 [2048], replicated, may hold values from 0.1 to 1.9
- switching_projector: bfloat16 [2048, 5632], P('sp', 'tp'), may hold values from -0.125 to 0.125
- widening_projector: bfloat16 [2048, 5632], P('sp', 'tp'), may hold values from -0.125 to 0.125
- shrinking_projector: bfloat16 [5632, 2048], P('tp', 'sp'), may hold values from -0.078125 to 0.078125
Outputs:
- layer_out: bfloat16 [12288, 2048], P(('sp', 'tp'))
The draws below stay inside these ranges and needn't reach their ends.
Inputs may be any that keep to these rules, and one draw needn't show every extreme that they name: `passage_label_per_token`: document numbers never fall along the sequence; a document holds at most 6144 positions.
All inputs are finite; a program needn't handle non-finite values.
Results may differ from the reference program's by a relative error of at most 0.014.
Values may be sent and summed in bfloat16 or wider, within the bound.
A program may use at most 128 MiB of HBM per device.

```python
import math
import jax
import jax.numpy as jnp
import numpy as np
from jax import lax

D = 2048
HEADS = 8
DK = 64
DV = 128
FF = 5632
BLOCK = 64
TOK_DEV = 768
TOKENS = 12288
DOCS = 4
DOC_MOST = 6144
N_SP = 16
N_TP = 2


def draw_lapse_preactivation(key, part):
    base_key, block_key = jax.random.split(jax.random.fold_in(key, 11))
    width = HEADS * DK
    noise = jax.random.normal(base_key, (TOKENS, width), jnp.float32)
    shift = jax.random.uniform(block_key, (TOKENS // TOK_DEV, 1, width), jnp.float32, -0.7, 0.7)
    shaped = noise.reshape(TOKENS // TOK_DEV, TOK_DEV, width) + shift
    return shaped.reshape(TOKENS, width).astype(jnp.bfloat16)


def draw_lapse_shift_entries(key, part):
    pick_key, slow_key, fast_key = jax.random.split(jax.random.fold_in(key, 23), 3)
    slow = jax.random.randint(pick_key, (HEADS,), 0, 2) > 0
    slow_vals = jnp.log(TOKENS / 16.0) + jax.random.uniform(slow_key, (HEADS, DK), jnp.float32, -1.0, 0.5)
    fast_vals = jax.random.uniform(fast_key, (HEADS, DK), jnp.float32, -0.5, 1.5)
    return jnp.where(slow[:, None], slow_vals, fast_vals).reshape(HEADS * DK).astype(jnp.float32)


def draw_surplus_attenuation_terms(key, part):
    where_key, size_key = jax.random.split(jax.random.fold_in(key, 37))
    number = max(TOKENS // TOK_DEV, 4)
    spots = jax.random.randint(where_key, (number,), 0, TOKENS)
    depth = jnp.log(jax.random.uniform(size_key, (number,), jnp.float32, 0.5, 0.8))
    return jnp.zeros((TOKENS,), jnp.float32).at[spots].min(depth)


def steps_of(stream_key, shape, pieces, low, largest):
    def one(axis_at, shards_of):
        heights = jax.random.uniform(jax.random.fold_in(jax.random.fold_in(stream_key, 6), axis_at), (shards_of,), jnp.float32, low / len(pieces), largest / len(pieces))
        return jnp.repeat(jnp.exp(heights), shape[axis_at] // shards_of).reshape((-1,) + (1,) * (len(shape) - axis_at - 1))

    factor_of = one(*pieces[0])
    for cut in pieces[1:]:
        factor_of = factor_of * one(*cut)
    return factor_of


def profile(number_of, total, most, skew):
    portions = [(1 << 20) // math.isqrt(standing ** skew) + 1 for standing in range(2, number_of + 1)]
    surplus, holding = total - most - (number_of - 1), [1] * (number_of - 1)
    while surplus > 0:
        movable = [i for i in range(number_of - 1) if holding[i] < most]
        mass, remaining = sum([portions[i] for i in movable]), surplus
        for i in movable:
            extra = min(most - holding[i], max(1, remaining * portions[i] // mass), surplus)
            holding[i] = holding[i] + extra
            surplus = surplus - extra
    return np.array([most] + holding)


def uneven(rng, number_of, total, limit, skew):
    if number_of == 2:
        one = jax.random.randint(rng, (), max(1, total - limit), min(limit, total - 1) + 1)
        return jnp.stack([one, total - one])
    lengths = jnp.asarray(profile(number_of, total, limit, skew), jnp.int32)
    twos = (number_of - 1) // 2
    giver, receiver = lengths[1:1 + 2 * twos:2], lengths[2:2 + 2 * twos:2]
    slack = jnp.minimum(giver - 1, limit - receiver)
    passed = jax.random.randint(jax.random.fold_in(rng, 1), (twos,), 0, 1 << 20) % (slack + 1)
    lengths = lengths.at[1:1 + 2 * twos:2].set(giver - passed).at[2:2 + 2 * twos:2].set(receiver + passed)
    return lengths[jax.random.permutation(jax.random.fold_in(rng, 2), number_of)]


def scatter_about(own_key, shape, scale, reach, cuts=(), kind=jnp.bfloat16):
    drawn = scale * jax.random.normal(own_key, shape, jnp.float32)
    if cuts:
        drawn = drawn * steps_of(own_key, shape, cuts, -0.22, 0.18)
    return jnp.clip(drawn, -reach, reach).astype(kind)


def setup_inputs(seed: int = 0) -> dict:
    splits = jax.random.split(jax.random.key(seed), 16)
    skip_connection_stream = scatter_about(splits[0], (TOKENS, D), 1.0, 6.0, ((0, 16),))
    probing_vectors = scatter_about(splits[1], (TOKENS, HEADS * DK), 1.0, 6.0, ((0, 16), (1, 2)))
    addressing_vectors = scatter_about(splits[2], (TOKENS, HEADS * DK), 1.0, 6.0, ((0, 16), (1, 2)))
    mapped_payloads = scatter_about(splits[3], (TOKENS, HEADS * DV), 1.0, 6.0, ((0, 16), (1, 2)))
    emission_switch = scatter_about(splits[4], (TOKENS, HEADS * DV), 1.0, 6.0, ((0, 16), (1, 2)))
    lapse_preactivation = draw_lapse_preactivation(jax.random.fold_in(splits[15], 71), 0)
    lapse_shift_entries = draw_lapse_shift_entries(jax.random.fold_in(splits[15], 71), 0)
    surplus_attenuation_terms = draw_surplus_attenuation_terms(jax.random.fold_in(splits[15], 71), 0)
    passage_label_per_token = jnp.searchsorted(jnp.cumsum(uneven(splits[8], DOCS, TOKENS, DOC_MOST, 1)), jnp.arange(TOKENS), side="right").astype(jnp.int32)
    attention_group_rescaler = jnp.clip(1.0 + 0.18 * jax.random.normal(splits[9], (DV,), jnp.float32), 0.1, 1.9)
    emission_projector = scatter_about(splits[10], (HEADS * DV, D), (HEADS * DV) ** -0.5, 0.1875, ((0, 2),))
    perceptron_rescaler = jnp.clip(1.0 + 0.18 * jax.random.normal(splits[11], (D,), jnp.float32), 0.1, 1.9)
    switching_projector = scatter_about(splits[12], (D, FF), D ** -0.5, 0.125, ((0, 16), (1, 2)))
    widening_projector = scatter_about(splits[13], (D, FF), D ** -0.5, 0.125, ((0, 16), (1, 2)))
    shrinking_projector = scatter_about(splits[14], (FF, D), FF ** -0.5, 0.078125, ((0, 2), (1, 16)))
    return {"skip_connection_stream": skip_connection_stream, "probing_vectors": probing_vectors, "addressing_vectors": addressing_vectors, "mapped_payloads": mapped_payloads, "emission_switch": emission_switch, "lapse_preactivation": lapse_preactivation, "lapse_shift_entries": lapse_shift_entries, "surplus_attenuation_terms": surplus_attenuation_terms, "passage_label_per_token": passage_label_per_token, "attention_group_rescaler": attention_group_rescaler, "emission_projector": emission_projector, "perceptron_rescaler": perceptron_rescaler, "switching_projector": switching_projector, "widening_projector": widening_projector, "shrinking_projector": shrinking_projector}


eps = 1e-06
sharpness_factor = 16.0

def head_split(array, heads):
    return array.reshape(array.shape[0], heads, -1).transpose(1, 0, 2)

def rounded(value):
    return lax.optimization_barrier(value.astype(jnp.bfloat16)).astype(jnp.float32)

def block_pass(query_head_rows, key_heads, value_heads, decay_heads, documents, recurrent_state, last_doc, offset, span):
    heads, length, _ = query_head_rows.shape
    blocks = length // span

    def to_blocks(array):
        return array.reshape(heads, blocks, span, array.shape[-1]).transpose(1, 0, 2, 3)
    lower = jnp.tril(jnp.ones((span, span), dtype=bool))

    def step(carry, inputs):
        recurrent_state, last_doc, offset = carry
        query_block, key_blk, value_block, piece_attenuation, doc_blk = inputs
        cumulative_decay = jnp.cumsum(piece_attenuation, axis=1)
        previous_valid = (doc_blk == last_doc).astype(jnp.float32)
        cross_block_output = jnp.einsum('gfl,glm->gfm', query_block * jnp.exp(cumulative_decay), recurrent_state, precision=lax.Precision.HIGHEST) * previous_valid[None, :, None]
        spread = cumulative_decay[:, :, None, :] - cumulative_decay[:, None, :, :]
        same = (doc_blk[:, None] == doc_blk[None, :]) & lower
        weights = jnp.exp(jnp.where(same[None, :, :, None], spread, -jnp.inf))
        scores = jnp.einsum('hik,hjk,hijk->hij', query_block, key_blk, weights, precision=lax.Precision.HIGHEST)
        result = cross_block_output + jnp.einsum('hij,hjv->hiv', scores, value_block, precision=lax.Precision.HIGHEST)
        final_memory_summary = cumulative_decay[:, -1, :]
        last_valid = (doc_blk[-1] == last_doc).astype(jnp.float32)
        tail_ok = (doc_blk == doc_blk[-1]).astype(jnp.float32)
        decayed_keys = key_blk * jnp.exp(final_memory_summary[:, None, :] - cumulative_decay) * tail_ok[None, :, None]
        recurrent_state = recurrent_state * jnp.exp(final_memory_summary)[:, :, None] * last_valid + jnp.einsum('wrz,wrs->wzs', decayed_keys, value_block, precision=lax.Precision.HIGHEST)
        return ((recurrent_state, doc_blk[-1], offset + final_memory_summary), (result, cumulative_decay + offset[:, None, :]))
    carry, outputs = lax.scan(step, (recurrent_state, last_doc, offset), (to_blocks(query_head_rows), to_blocks(key_heads), to_blocks(value_heads), to_blocks(decay_heads), documents.reshape(blocks, span)))
    result, running_state = outputs
    result = result.transpose(1, 0, 2, 3).reshape(heads, length, -1)
    running_state = running_state.transpose(1, 0, 2, 3).reshape(heads, length, -1)
    return (carry[0], carry[2], result, running_state)

def reference(skip_connection_stream, probing_vectors, addressing_vectors, mapped_payloads, emission_switch, lapse_preactivation, lapse_shift_entries, surplus_attenuation_terms, passage_label_per_token, attention_group_rescaler, emission_projector, perceptron_rescaler, switching_projector, widening_projector, shrinking_projector):
    keeping_exponent = jax.nn.log_sigmoid(lapse_preactivation.astype(jnp.float32) + lapse_shift_entries[None, :]) / sharpness_factor + surplus_attenuation_terms[:, None]
    query_head_rows = head_split(probing_vectors.astype(jnp.float32) * DK ** (-0.5), HEADS)
    key_heads = head_split(addressing_vectors.astype(jnp.float32), HEADS)
    value_heads = head_split(mapped_payloads.astype(jnp.float32), HEADS)
    decay_heads = head_split(keeping_exponent, HEADS)
    zero_state = jnp.zeros((HEADS, DK, DV), jnp.float32)
    _, _, attn, _ = block_pass(query_head_rows, key_heads, value_heads, decay_heads, passage_label_per_token, zero_state, jnp.array(-1, jnp.int32), jnp.zeros((HEADS, DK), jnp.float32), BLOCK)
    normed_attn = attn * lax.rsqrt(lax.optimization_barrier(jnp.mean(attn * attn, axis=-1, keepdims=True)) + eps) * attention_group_rescaler
    flat = normed_attn.transpose(1, 0, 2).reshape(attn.shape[1], HEADS * DV)
    gated = (flat * jax.nn.silu(emission_switch.astype(jnp.float32))).astype(jnp.bfloat16)
    head_cols = HEADS * DV // N_TP
    ff_cols = FF // N_TP

    def rows_fn(index):
        start = (index * TOK_DEV).astype(jnp.int32)
        gated_rows = lax.dynamic_slice_in_dim(gated, start, TOK_DEV, 0)
        resid_rows = lax.dynamic_slice_in_dim(skip_connection_stream, start, TOK_DEV, 0)
        mixed = jnp.zeros((TOK_DEV, D), jnp.float32)
        for group in range(N_TP):
            mixed = mixed + rounded(jnp.dot(gated_rows[:, group * head_cols:(group + 1) * head_cols], emission_projector[group * head_cols:(group + 1) * head_cols], preferred_element_type=jnp.float32))
        first_resid = (resid_rows.astype(jnp.float32) + mixed).astype(jnp.bfloat16)
        wide = first_resid.astype(jnp.float32)
        normed = (wide * lax.rsqrt(lax.optimization_barrier(jnp.mean(wide * wide, axis=-1, keepdims=True)) + eps) * perceptron_rescaler).astype(jnp.bfloat16)
        gate = jnp.dot(normed, switching_projector, preferred_element_type=jnp.float32)
        upper = jnp.dot(normed, widening_projector, preferred_element_type=jnp.float32)
        hidden = (jax.nn.silu(gate) * upper).astype(jnp.bfloat16)
        ffn_out = jnp.zeros((TOK_DEV, D), jnp.float32)
        for group in range(N_TP):
            ffn_out = ffn_out + rounded(jnp.dot(hidden[:, group * ff_cols:(group + 1) * ff_cols], shrinking_projector[group * ff_cols:(group + 1) * ff_cols], preferred_element_type=jnp.float32))
        return (wide + 0.5 * ffn_out).astype(jnp.bfloat16)
    blocks_out = lax.map(rows_fn, jnp.arange(N_SP, dtype=jnp.int32))
    return blocks_out.reshape(N_SP * TOK_DEV, D)
```

```python
import functools

import jax
import jax.numpy as jnp
from jax import lax
from jax.experimental import pallas as pl
from jax.experimental.pallas import tpu as pltpu
from jax.sharding import PartitionSpec as P

DK = 64
DV = 128
BLOCK = 64
LIMIT = 80.0

eps = 1e-06
sharpness_factor = 16.0
HIGHEST = lax.Precision.HIGHEST
F32 = jnp.float32
BF16 = jnp.bfloat16


def dot0(a, b, precision=None):
    return lax.dot_general(
        a, b, (((0,), (0,)), ((), ())), precision=precision, preferred_element_type=F32
    )


def dot1(a, b, precision=None):
    return lax.dot_general(
        a, b, (((1,), (0,)), ((), ())), precision=precision, preferred_element_type=F32
    )


def local_pass(
    q_ref, k_ref, v_ref, lapse_ref, shift_ref, surplus_ref, doc_col_ref, doc_row_ref,
    out_ref, qrun_ref, state_ref, total_ref,
):
    length, width = q_ref.shape
    heads = width // DK
    span = BLOCK
    middle = span // 2
    rows = lax.broadcasted_iota(jnp.int32, (span, span), 0)
    cols = lax.broadcasted_iota(jnp.int32, (span, span), 1)
    lower = rows >= cols
    tril = lower.astype(F32)
    ones = jnp.ones((span, DV), F32)
    lane_head = lax.broadcasted_iota(jnp.int32, (span, width), 1) // DK
    head_mask = [(lane_head == h).astype(F32) for h in range(heads)]

    def per_head(a):
        return jnp.concatenate([(a * m).astype(BF16) for m in head_mask], axis=0)

    state = None
    offset = jnp.zeros((1, width), F32)
    for b in range(length // span):
        at = pl.ds(b * span, span)
        pre = lapse_ref[at, :].astype(F32) + shift_ref[...]
        ld = (jnp.minimum(pre, 0.0) - jnp.log1p(jnp.exp(-jnp.abs(pre)))) * (
            1.0 / sharpness_factor
        ) + surplus_ref[at, :]
        cum = dot1(tril, ld, HIGHEST)
        q = q_ref[at, :].astype(F32) * DK ** (-0.5)
        k = k_ref[at, :].astype(F32)
        v = v_ref[at, :]
        doc_col = doc_col_ref[at, :]
        doc_row = doc_row_ref[b : b + 1, :]
        tot = cum[span - 1 : span, :]
        centre = cum[middle : middle + 1, :]
        decayed = jnp.exp(cum)
        qd = q * decayed
        qrun_ref[at, :] = (qd * jnp.exp(offset)).astype(BF16)
        qs = q * jnp.exp(jnp.minimum(cum - centre, LIMIT))
        ks = (k * jnp.exp(jnp.minimum(centre - cum, LIMIT))).astype(BF16)
        scores = lax.dot_general(
            per_head(qs), ks, (((1,), (1,)), ((), ())), preferred_element_type=F32
        )
        same = (doc_col == doc_row) & lower
        if b > 0:
            last = doc_col_ref[b * span - 1 : b * span, :]
            valid = (doc_col == last).astype(F32)
            cross = dot1(per_head(qd), state.astype(BF16))
        for h in range(heads):
            piece = slice(h * span, (h + 1) * span)
            lanes = slice(h * DV, (h + 1) * DV)
            masked = jnp.where(same, scores[piece], 0.0).astype(BF16)
            res = dot1(masked, v[:, lanes])
            if b > 0:
                res = res + cross[piece] * valid
            out_ref[at, lanes] = res
        tail_doc = doc_col[span - 1 : span, :]
        tail_ok = (doc_col == tail_doc).astype(F32)
        kd = (k * jnp.exp(tot - cum) * tail_ok).astype(BF16)
        update = dot0(kd, v)
        update = jnp.concatenate(
            [update[h * DK : (h + 1) * DK, h * DV : (h + 1) * DV] for h in range(heads)], axis=0
        )
        if b > 0:
            keep = (tail_doc == last).astype(F32)
            state = state * (jnp.exp(dot0(ld, ones, HIGHEST)) * keep) + update
        else:
            state = update
        offset = offset + tot
    state_ref[...] = state
    total_ref[...] = offset


def finish_pass(out_ref, qrun_ref, entering_ref, reaches_ref, switch_ref, gain_ref, gated_ref):
    length, width = qrun_ref.shape
    heads = width // DK
    rows = 256 if length % 256 == 0 else length
    lane_head = lax.broadcasted_iota(jnp.int32, (rows, width), 1) // DK
    for r in range(length // rows):
        at = pl.ds(r * rows, rows)
        q = qrun_ref[at, :]
        reaches = reaches_ref[at, :]
        for h in range(heads):
            lanes = slice(h * DV, (h + 1) * DV)
            qh = jnp.where(lane_head == h, q, jnp.zeros_like(q))
            attn = out_ref[at, lanes] + dot1(qh, entering_ref[...]) * reaches
            normed = (
                attn
                * lax.rsqrt(jnp.mean(attn * attn, axis=-1, keepdims=True) + eps)
                * gain_ref[...]
            )
            s = switch_ref[at, lanes].astype(F32)
            gated_ref[at, lanes] = (normed * (s / (1.0 + jnp.exp(-s)))).astype(BF16)


def rms_rows(rows, gain):
    wide = rows.astype(F32)
    return (wide * lax.rsqrt(jnp.mean(wide * wide, axis=-1, keepdims=True) + eps) * gain).astype(
        BF16
    )


def vmem(n):
    return [pl.BlockSpec(memory_space=pltpu.VMEM)] * n


def per_device(
    skip_connection_stream,
    probing_vectors,
    addressing_vectors,
    mapped_payloads,
    emission_switch,
    lapse_preactivation,
    lapse_shift_entries,
    surplus_attenuation_terms,
    passage_label_per_token,
    attention_group_rescaler,
    emission_projector,
    perceptron_rescaler,
    switching_projector,
    widening_projector,
    shrinking_projector,
):
    rows_here, width = probing_vectors.shape
    heads = width // DK
    n_sp, n_tp = lax.axis_size("sp"), lax.axis_size("tp")
    place, group = lax.axis_index("sp"), lax.axis_index("tp")
    docs = passage_label_per_token

    def to_later(a, step):
        return lax.ppermute(a, "tp", [(i, (i + step) % n_tp) for i in range(n_tp)])

    gate_w = lax.all_gather(switching_projector, "sp", axis=0, tiled=True)
    up_w = lax.all_gather(widening_projector, "sp", axis=0, tiled=True)
    down_w = lax.all_gather(shrinking_projector, "sp", axis=1, tiled=True)
    projectors = [emission_projector] + [to_later(emission_projector, s) for s in range(1, n_tp)]

    local_out, qrun, state, total = pl.pallas_call(
        local_pass,
        out_shape=(
            jax.ShapeDtypeStruct((rows_here, heads * DV), F32),
            jax.ShapeDtypeStruct((rows_here, width), BF16),
            jax.ShapeDtypeStruct((width, DV), F32),
            jax.ShapeDtypeStruct((1, width), F32),
        ),
        in_specs=vmem(8),
        out_specs=tuple(vmem(4)),
        cost_estimate=pl.CostEstimate(
            flops=40_000_000_000, bytes_accessed=6_000_000, transcendentals=0
        ),
        name="local_pass",
    )(
        probing_vectors,
        addressing_vectors,
        mapped_payloads,
        lapse_preactivation,
        lapse_shift_entries[None, :],
        surplus_attenuation_terms[:, None],
        docs[:, None],
        docs.reshape(-1, BLOCK),
    )

    unbroken = (docs[0] == docs[-1]).astype(F32)
    ends = jnp.stack([docs[0], docs[-1]]).astype(BF16)
    small = jnp.concatenate([(jnp.exp(total[0]) * unbroken).astype(BF16), ends])
    tail_rows = 16 * pl.cdiv(small.size, 16 * DV)
    small = jnp.pad(small, (0, tail_rows * DV - small.size)).reshape(tail_rows, DV)
    packed = jnp.concatenate([state.astype(BF16), small], axis=0)
    half = (width + tail_rows) // 2
    first_half = lax.all_gather(packed[:half], "sp")
    packed, first_half = lax.optimization_barrier((packed, first_half))
    packed = jnp.concatenate([first_half, lax.all_gather(packed[half:], "sp")], axis=1)
    states = packed[:, :width]
    smalls = packed[:, width:].reshape(n_sp, -1).astype(F32)
    decays, first_doc, last_doc = smalls[:, :width], smalls[:, width], smalls[:, width + 1]
    before = jnp.concatenate([jnp.full((1,), -1.0, F32), last_doc[:-1]])
    decays = decays * (before == first_doc).astype(F32)[:, None]
    entering = jnp.zeros((width, DV), F32)
    for j in range(n_sp):
        entering = jnp.where(
            j < place, entering * decays[j][:, None] + states[j].astype(F32), entering
        )
    reaches = (docs.astype(F32) == before[place]).astype(F32)

    gated = pl.pallas_call(
        finish_pass,
        out_shape=jax.ShapeDtypeStruct((rows_here, heads * DV), BF16),
        in_specs=vmem(6),
        out_specs=vmem(1)[0],
        cost_estimate=pl.CostEstimate(
            flops=5_000_000_000, bytes_accessed=5_000_000, transcendentals=0
        ),
        name="finish_pass",
    )(
        local_out,
        qrun,
        entering.astype(BF16),
        reaches[:, None],
        emission_switch,
        attention_group_rescaler[None, :],
    )

    gateds = [gated] + [to_later(gated, s) for s in range(1, n_tp)]
    mixed = jnp.zeros((), F32)
    for rows, weight in zip(gateds, projectors):
        part = jnp.dot(rows, weight, preferred_element_type=F32).astype(BF16)
        mixed = mixed + part.astype(F32)
    first_all = (skip_connection_stream.astype(F32) + mixed).astype(BF16)
    normed = rms_rows(first_all, perceptron_rescaler)
    gate = jnp.dot(normed, gate_w, preferred_element_type=F32)
    upper = jnp.dot(normed, up_w, preferred_element_type=F32)
    hidden = (jax.nn.silu(gate) * upper).astype(BF16)

    share = rows_here // n_tp

    def share_of(a, owner):
        return lax.dynamic_slice_in_dim(a, owner * share, share, 0)

    def down(owner):
        return jnp.dot(share_of(hidden, owner), down_w, preferred_element_type=F32).astype(BF16)

    arrived = [to_later(down((group + s) % n_tp), s) for s in range(1, n_tp)]
    ffn_out = down(group).astype(F32)
    for part in arrived:
        ffn_out = ffn_out + part.astype(F32)
    first_own = share_of(first_all, group).astype(F32)
    return (first_own + 0.5 * ffn_out).astype(BF16)


def solution(mesh):
    placed = (
        P("sp", None),
        P("sp", "tp"),
        P("sp", "tp"),
        P("sp", "tp"),
        P("sp", "tp"),
        P("sp", "tp"),
        P("tp"),
        P("sp"),
        P("sp"),
        P(),
        P("tp", None),
        P(),
        P("sp", "tp"),
        P("sp", "tp"),
        P("tp", "sp"),
    )
    return jax.shard_map(
        per_device, mesh=mesh, in_specs=placed, out_specs=P(("sp", "tp"), None), check_vma=False
    )
```

```python
import functools

import jax
import jax.numpy as jnp
from jax import lax
from jax.experimental import pallas as pl
from jax.experimental.pallas import tpu as pltpu
from jax.sharding import PartitionSpec as P

DK = 64
DV = 128
BLOCK = 64
LIMIT = 80.0

eps = 1e-06
sharpness_factor = 16.0
HIGHEST = lax.Precision.HIGHEST
F32 = jnp.float32
BF16 = jnp.bfloat16


def dot0(a, b, precision=None):
    return lax.dot_general(
        a, b, (((0,), (0,)), ((), ())), precision=precision, preferred_element_type=F32
    )


def dot1(a, b, precision=None):
    return lax.dot_general(
        a, b, (((1,), (0,)), ((), ())), precision=precision, preferred_element_type=F32
    )


def local_pass(
    q_ref, k_ref, v_ref, lapse_ref, shift_ref, surplus_ref, doc_col_ref, doc_row_ref,
    out_ref, qrun_ref, state_ref, total_ref,
):
    length, width = q_ref.shape
    heads = width // DK
    span = BLOCK
    middle = span // 2
    rows = lax.broadcasted_iota(jnp.int32, (span, span), 0)
    cols = lax.broadcasted_iota(jnp.int32, (span, span), 1)
    lower = rows >= cols
    tril = lower.astype(F32)
    ones = jnp.ones((span, DV), F32)
    lane_head = lax.broadcasted_iota(jnp.int32, (span, width), 1) // DK
    head_mask = [(lane_head == h).astype(F32) for h in range(heads)]

    def per_head(a):
        return jnp.concatenate([(a * m).astype(BF16) for m in head_mask], axis=0)

    state = None
    offset = jnp.zeros((1, width), F32)
    for b in range(length // span):
        at = pl.ds(b * span, span)
        pre = lapse_ref[at, :].astype(F32) + shift_ref[...]
        ld = (jnp.minimum(pre, 0.0) - jnp.log1p(jnp.exp(-jnp.abs(pre)))) * (
            1.0 / sharpness_factor
        ) + surplus_ref[at, :]
        cum = dot1(tril, ld, HIGHEST)
        q = q_ref[at, :].astype(F32) * DK ** (-0.5)
        k = k_ref[at, :].astype(F32)
        v = v_ref[at, :]
        doc_col = doc_col_ref[at, :]
        doc_row = doc_row_ref[b : b + 1, :]
        tot = cum[span - 1 : span, :]
        centre = cum[middle : middle + 1, :]
        decayed = jnp.exp(cum)
        qd = q * decayed
        qrun_ref[at, :] = (qd * jnp.exp(offset)).astype(BF16)
        qs = q * jnp.exp(jnp.minimum(cum - centre, LIMIT))
        ks = (k * jnp.exp(jnp.minimum(centre - cum, LIMIT))).astype(BF16)
        scores = lax.dot_general(
            per_head(qs), ks, (((1,), (1,)), ((), ())), preferred_element_type=F32
        )
        same = (doc_col == doc_row) & lower
        if b > 0:
            last = doc_col_ref[b * span - 1 : b * span, :]
            valid = (doc_col == last).astype(F32)
            cross = dot1(per_head(qd), state.astype(BF16))
        for h in range(heads):
            piece = slice(h * span, (h + 1) * span)
            lanes = slice(h * DV, (h + 1) * DV)
            masked = jnp.where(same, scores[piece], 0.0).astype(BF16)
            res = dot1(masked, v[:, lanes])
            if b > 0:
                res = res + cross[piece] * valid
            out_ref[at, lanes] = res
        tail_doc = doc_col[span - 1 : span, :]
        tail_ok = (doc_col == tail_doc).astype(F32)
        kd = (k * jnp.exp(tot - cum) * tail_ok).astype(BF16)
        update = dot0(kd, v)
        update = jnp.concatenate(
            [update[h * DK : (h + 1) * DK, h * DV : (h + 1) * DV] for h in range(heads)], axis=0
        )
        if b > 0:
            keep = (tail_doc == last).astype(F32)
            state = state * (jnp.exp(dot0(ld, ones, HIGHEST)) * keep) + update
        else:
            state = update
        offset = offset + tot
    state_ref[...] = state
    total_ref[...] = offset


def finish_pass(out_ref, qrun_ref, entering_ref, reaches_ref, switch_ref, gain_ref, gated_ref):
    length, width = qrun_ref.shape
    heads = width // DK
    rows = 256 if length % 256 == 0 else length
    lane_head = lax.broadcasted_iota(jnp.int32, (rows, width), 1) // DK
    for r in range(length // rows):
        at = pl.ds(r * rows, rows)
        q = qrun_ref[at, :]
        reaches = reaches_ref[at, :]
        for h in range(heads):
            lanes = slice(h * DV, (h + 1) * DV)
            qh = jnp.where(lane_head == h, q, jnp.zeros_like(q))
            attn = out_ref[at, lanes] + dot1(qh, entering_ref[...]) * reaches
            normed = (
                attn
                * lax.rsqrt(jnp.mean(attn * attn, axis=-1, keepdims=True) + eps)
                * gain_ref[...]
            )
            s = switch_ref[at, lanes].astype(F32)
            gated_ref[at, lanes] = (normed * (s / (1.0 + jnp.exp(-s)))).astype(BF16)


def rms_rows(rows, gain):
    wide = rows.astype(F32)
    return (wide * lax.rsqrt(jnp.mean(wide * wide, axis=-1, keepdims=True) + eps) * gain).astype(
        BF16
    )


def ring_orders(n_sp):
    chips = n_sp // 2
    return list(range(0, chips, 2)) + list(range(1, chips, 2))[::-1]


def ring_pairs(n_sp, step):
    ring = ring_orders(n_sp)
    count = len(ring)
    return [
        (2 * ring[i] + core, 2 * ring[(i + step) % count] + core)
        for i in range(count)
        for core in (0, 1)
    ]


def swap_cores(a, n_sp):
    return lax.ppermute(a, "sp", [(i, i ^ 1) for i in range(n_sp)])


def ring_start(own, n_sp):
    return (
        lax.ppermute(own, "sp", ring_pairs(n_sp, 1)),
        lax.ppermute(own, "sp", ring_pairs(n_sp, -1)),
    )


def ring_rest(first, n_sp, axis):
    behind, ahead = [first[0]], [first[1]]
    count = n_sp // 2
    for _ in range((count - 1) // 2 - 1):
        behind.append(lax.ppermute(behind[-1], "sp", ring_pairs(n_sp, 1)))
        ahead.append(lax.ppermute(ahead[-1], "sp", ring_pairs(n_sp, -1)))
    size = first[0].shape[axis] // 2
    low = lax.slice_in_dim(behind[-1], 0, size, axis=axis)
    high = lax.slice_in_dim(ahead[-1], size, 2 * size, axis=axis)
    low = lax.ppermute(low, "sp", ring_pairs(n_sp, 1))
    high = lax.ppermute(high, "sp", ring_pairs(n_sp, -1))
    return behind, ahead, (low, high)


def vmem(n):
    return [pl.BlockSpec(memory_space=pltpu.VMEM)] * n


def per_device(
    skip_connection_stream,
    probing_vectors,
    addressing_vectors,
    mapped_payloads,
    emission_switch,
    lapse_preactivation,
    lapse_shift_entries,
    surplus_attenuation_terms,
    passage_label_per_token,
    attention_group_rescaler,
    emission_projector,
    perceptron_rescaler,
    switching_projector,
    widening_projector,
    shrinking_projector,
):
    rows_here, width = probing_vectors.shape
    heads = width // DK
    n_sp, n_tp = lax.axis_size("sp"), lax.axis_size("tp")
    place, group = lax.axis_index("sp"), lax.axis_index("tp")
    docs = passage_label_per_token

    def to_later(a, step):
        return lax.ppermute(a, "tp", [(i, (i + step) % n_tp) for i in range(n_tp)])

    both_w = jnp.concatenate([switching_projector, widening_projector], axis=1)
    both_first = ring_start(both_w, n_sp)
    down_first = ring_start(shrinking_projector, n_sp)
    projectors = [emission_projector] + [to_later(emission_projector, s) for s in range(1, n_tp)]

    local_out, qrun, state, total = pl.pallas_call(
        local_pass,
        out_shape=(
            jax.ShapeDtypeStruct((rows_here, heads * DV), F32),
            jax.ShapeDtypeStruct((rows_here, width), BF16),
            jax.ShapeDtypeStruct((width, DV), F32),
            jax.ShapeDtypeStruct((1, width), F32),
        ),
        in_specs=vmem(8),
        out_specs=tuple(vmem(4)),
        cost_estimate=pl.CostEstimate(
            flops=40_000_000_000, bytes_accessed=6_000_000, transcendentals=0
        ),
        name="local_pass",
    )(
        probing_vectors,
        addressing_vectors,
        mapped_payloads,
        lapse_preactivation,
        lapse_shift_entries[None, :],
        surplus_attenuation_terms[:, None],
        docs[:, None],
        docs.reshape(-1, BLOCK),
    )

    unbroken = (docs[0] == docs[-1]).astype(F32)
    ends = jnp.stack([docs[0], docs[-1]]).astype(BF16)
    small = jnp.concatenate([(jnp.exp(total[0]) * unbroken).astype(BF16), ends])
    tail_rows = 16 * pl.cdiv(small.size, 16 * DV)
    small = jnp.pad(small, (0, tail_rows * DV - small.size)).reshape(tail_rows, DV)
    packed = jnp.concatenate([state.astype(BF16), small], axis=0)
    half = (width + tail_rows) // 2
    first_half = lax.all_gather(packed[:half], "sp")
    packed, first_half = lax.optimization_barrier((packed, first_half))
    second_half = lax.all_gather(packed[half:], "sp")
    second_half, both_first = lax.optimization_barrier((second_half, both_first))
    packed = jnp.concatenate([first_half, second_half], axis=1)
    behind, ahead, opposite = ring_rest(both_first, n_sp, 1)
    down_first, opposite = lax.optimization_barrier((down_first, opposite))
    down_behind, down_ahead, down_opposite = ring_rest(down_first, n_sp, 0)

    ring = jnp.asarray(ring_orders(n_sp), jnp.int32)
    count = n_sp // 2
    spot = jnp.argmax(ring == place // 2)
    core = place % 2

    def chip_at(steps_behind):
        return ring[(spot - steps_behind + count) % count]

    chips = [chip_at(0)]
    chips += [chip_at(d + 1) for d in range(len(behind))]
    chips += [chip_at(-d - 1) for d in range(len(ahead))]
    chips += [chip_at(count // 2)]
    owners = [2 * c + core for c in chips] + [2 * c + 1 - core for c in chips]
    lows, highs = opposite
    here = [both_w] + behind + ahead + [jnp.concatenate([lows, highs], axis=1)]
    there = [swap_cores(a, n_sp) for a in [both_w] + behind + ahead]
    there += [jnp.concatenate([swap_cores(lows, n_sp), swap_cores(highs, n_sp)], axis=1)]
    hidden_width = switching_projector.shape[1]
    gate_w = jnp.concatenate([a[:, :hidden_width] for a in here + there], axis=0)
    up_w = jnp.concatenate([a[:, hidden_width:] for a in here + there], axis=0)
    down_here = [shrinking_projector] + down_behind + down_ahead
    down_there = [swap_cores(a, n_sp) for a in down_here]
    states = packed[:, :width]
    smalls = packed[:, width:].reshape(n_sp, -1).astype(F32)
    decays, first_doc, last_doc = smalls[:, :width], smalls[:, width], smalls[:, width + 1]
    before = jnp.concatenate([jnp.full((1,), -1.0, F32), last_doc[:-1]])
    decays = decays * (before == first_doc).astype(F32)[:, None]
    entering = jnp.zeros((width, DV), F32)
    for j in range(n_sp):
        entering = jnp.where(
            j < place, entering * decays[j][:, None] + states[j].astype(F32), entering
        )
    reaches = (docs.astype(F32) == before[place]).astype(F32)

    gated = pl.pallas_call(
        finish_pass,
        out_shape=jax.ShapeDtypeStruct((rows_here, heads * DV), BF16),
        in_specs=vmem(6),
        out_specs=vmem(1)[0],
        cost_estimate=pl.CostEstimate(
            flops=5_000_000_000, bytes_accessed=5_000_000, transcendentals=0
        ),
        name="finish_pass",
    )(
        local_out,
        qrun,
        entering.astype(BF16),
        reaches[:, None],
        emission_switch,
        attention_group_rescaler[None, :],
    )

    gateds = [gated] + [to_later(gated, s) for s in range(1, n_tp)]
    mixed = jnp.zeros((), F32)
    for rows, weight in zip(gateds, projectors):
        part = jnp.dot(rows, weight, preferred_element_type=F32).astype(BF16)
        mixed = mixed + part.astype(F32)
    first_all = (skip_connection_stream.astype(F32) + mixed).astype(BF16)
    normed = rms_rows(first_all, perceptron_rescaler)
    block = switching_projector.shape[0]

    def columns(a, owner):
        return lax.dynamic_slice_in_dim(a, owner * block, block, 1)

    ringed = jnp.concatenate([columns(normed, owner) for owner in owners], axis=1)
    gate = jnp.dot(ringed, gate_w, preferred_element_type=F32)
    upper = jnp.dot(ringed, up_w, preferred_element_type=F32)
    hidden = (jax.nn.silu(gate) * upper).astype(BF16)

    share = rows_here // n_tp

    def share_of(a, owner):
        return lax.dynamic_slice_in_dim(a, owner * share, share, 0)

    def reduced(weight):
        def down(owner):
            return jnp.dot(share_of(hidden, owner), weight, preferred_element_type=F32).astype(BF16)

        arrived = [to_later(down((group + s) % n_tp), s) for s in range(1, n_tp)]
        total = down(group).astype(F32)
        for part in arrived:
            total = total + part.astype(F32)
        return total

    late_here = jnp.concatenate(down_opposite, axis=0)
    late_there = jnp.concatenate([swap_cores(a, n_sp) for a in down_opposite], axis=0)
    near = (len(down_here) + 1) // 2
    order = [0] + [i + 1 + j * len(down_behind) for i in range(len(down_behind)) for j in (0, 1)]
    groups = [order[:near], order[near:], [len(down_here)]]
    down_here, down_there = down_here + [late_here], down_there + [late_there]
    first_own = share_of(first_all, group)
    out = first_own
    for members in groups:
        weight = jnp.concatenate(
            [down_here[i] for i in members] + [down_there[i] for i in members], axis=1
        )
        whose = [owners[i] for i in members] + [owners[len(chips) + i] for i in members]
        total = reduced(weight)
        for i, owner in enumerate(whose):
            start = (0, owner * block)
            piece = total[:, i * block : (i + 1) * block]
            base = lax.dynamic_slice(first_own, start, (share, block)).astype(F32)
            out = lax.dynamic_update_slice(out, (base + 0.5 * piece).astype(BF16), start)
    return out


def solution(mesh):
    placed = (
        P("sp", None),
        P("sp", "tp"),
        P("sp", "tp"),
        P("sp", "tp"),
        P("sp", "tp"),
        P("sp", "tp"),
        P("tp"),
        P("sp"),
        P("sp"),
        P(),
        P("tp", None),
        P(),
        P("sp", "tp"),
        P("sp", "tp"),
        P("tp", "sp"),
    )
    return jax.shard_map(
        per_device, mesh=mesh, in_specs=placed, out_specs=P(("sp", "tp"), None), check_vma=False
    )
```

```python
import functools

import jax
import jax.numpy as jnp
from jax import lax
from jax.experimental import pallas as pl
from jax.experimental.pallas import tpu as pltpu
from jax.sharding import PartitionSpec as P

DK = 64
DV = 128
BLOCK = 64
LIMIT = 80.0

eps = 1e-06
sharpness_factor = 16.0
HIGHEST = lax.Precision.HIGHEST
F32 = jnp.float32
BF16 = jnp.bfloat16


def dot0(a, b, precision=None):
    return lax.dot_general(
        a, b, (((0,), (0,)), ((), ())), precision=precision, preferred_element_type=F32
    )


def dot1(a, b, precision=None):
    return lax.dot_general(
        a, b, (((1,), (0,)), ((), ())), precision=precision, preferred_element_type=F32
    )


def local_pass(
    q_ref, k_ref, v_ref, lapse_ref, shift_ref, surplus_ref, doc_col_ref, doc_row_ref,
    out_ref, qrun_ref, state_ref, total_ref,
):
    length, width = q_ref.shape
    heads = width // DK
    span = BLOCK
    middle = span // 2
    rows = lax.broadcasted_iota(jnp.int32, (span, span), 0)
    cols = lax.broadcasted_iota(jnp.int32, (span, span), 1)
    lower = rows >= cols
    tril = lower.astype(F32)
    ones = jnp.ones((span, DV), F32)
    lane_head = lax.broadcasted_iota(jnp.int32, (span, width), 1) // DK
    head_mask = [(lane_head == h).astype(F32) for h in range(heads)]

    def per_head(a):
        return jnp.concatenate([(a * m).astype(BF16) for m in head_mask], axis=0)

    state = None
    offset = jnp.zeros((1, width), F32)
    for b in range(length // span):
        at = pl.ds(b * span, span)
        pre = lapse_ref[at, :].astype(F32) + shift_ref[...]
        ld = (jnp.minimum(pre, 0.0) - jnp.log1p(jnp.exp(-jnp.abs(pre)))) * (
            1.0 / sharpness_factor
        ) + surplus_ref[at, :]
        cum = dot1(tril, ld, HIGHEST)
        q = q_ref[at, :].astype(F32) * DK ** (-0.5)
        k = k_ref[at, :].astype(F32)
        v = v_ref[at, :]
        doc_col = doc_col_ref[at, :]
        doc_row = doc_row_ref[b : b + 1, :]
        tot = cum[span - 1 : span, :]
        centre = cum[middle : middle + 1, :]
        decayed = jnp.exp(cum)
        qd = q * decayed
        qrun_ref[at, :] = (qd * jnp.exp(offset)).astype(BF16)
        qs = q * jnp.exp(jnp.minimum(cum - centre, LIMIT))
        ks = (k * jnp.exp(jnp.minimum(centre - cum, LIMIT))).astype(BF16)
        scores = lax.dot_general(
            per_head(qs), ks, (((1,), (1,)), ((), ())), preferred_element_type=F32
        )
        same = (doc_col == doc_row) & lower
        if b > 0:
            last = doc_col_ref[b * span - 1 : b * span, :]
            valid = (doc_col == last).astype(F32)
            cross = dot1(per_head(qd), state.astype(BF16))
        for h in range(heads):
            piece = slice(h * span, (h + 1) * span)
            lanes = slice(h * DV, (h + 1) * DV)
            masked = jnp.where(same, scores[piece], 0.0).astype(BF16)
            res = dot1(masked, v[:, lanes])
            if b > 0:
                res = res + cross[piece] * valid
            out_ref[at, lanes] = res
        tail_doc = doc_col[span - 1 : span, :]
        tail_ok = (doc_col == tail_doc).astype(F32)
        kd = (k * jnp.exp(tot - cum) * tail_ok).astype(BF16)
        update = dot0(kd, v)
        update = jnp.concatenate(
            [update[h * DK : (h + 1) * DK, h * DV : (h + 1) * DV] for h in range(heads)], axis=0
        )
        if b > 0:
            keep = (tail_doc == last).astype(F32)
            state = state * (jnp.exp(dot0(ld, ones, HIGHEST)) * keep) + update
        else:
            state = update
        offset = offset + tot
    state_ref[...] = state
    total_ref[...] = offset


def finish_pass(out_ref, qrun_ref, entering_ref, reaches_ref, switch_ref, gain_ref, gated_ref):
    length, width = qrun_ref.shape
    heads = width // DK
    rows = 256 if length % 256 == 0 else length
    lane_head = lax.broadcasted_iota(jnp.int32, (rows, width), 1) // DK
    for r in range(length // rows):
        at = pl.ds(r * rows, rows)
        q = qrun_ref[at, :]
        reaches = reaches_ref[at, :]
        for h in range(heads):
            lanes = slice(h * DV, (h + 1) * DV)
            qh = jnp.where(lane_head == h, q, jnp.zeros_like(q))
            attn = out_ref[at, lanes] + dot1(qh, entering_ref[...]) * reaches
            normed = (
                attn
                * lax.rsqrt(jnp.mean(attn * attn, axis=-1, keepdims=True) + eps)
                * gain_ref[...]
            )
            s = switch_ref[at, lanes].astype(F32)
            gated_ref[at, lanes] = (normed * (s / (1.0 + jnp.exp(-s)))).astype(BF16)


def rms_rows(rows, gain):
    wide = rows.astype(F32)
    return (wide * lax.rsqrt(jnp.mean(wide * wide, axis=-1, keepdims=True) + eps) * gain).astype(
        BF16
    )


def ring_orders(n_sp):
    chips = n_sp // 2
    return list(range(0, chips, 2)) + list(range(1, chips, 2))[::-1]


def ring_pairs(n_sp, step):
    ring = ring_orders(n_sp)
    count = len(ring)
    return [
        (2 * ring[i] + core, 2 * ring[(i + step) % count] + core)
        for i in range(count)
        for core in (0, 1)
    ]


def swap_cores(a, n_sp):
    return lax.ppermute(a, "sp", [(i, i ^ 1) for i in range(n_sp)])


def ring_start(own, n_sp):
    return (
        lax.ppermute(own, "sp", ring_pairs(n_sp, 1)),
        lax.ppermute(own, "sp", ring_pairs(n_sp, -1)),
    )


def ring_rest(first, n_sp, axis):
    behind, ahead = [first[0]], [first[1]]
    count = n_sp // 2
    for _ in range((count - 1) // 2 - 1):
        behind.append(lax.ppermute(behind[-1], "sp", ring_pairs(n_sp, 1)))
        ahead.append(lax.ppermute(ahead[-1], "sp", ring_pairs(n_sp, -1)))
    size = first[0].shape[axis] // 2
    low = lax.slice_in_dim(behind[-1], 0, size, axis=axis)
    high = lax.slice_in_dim(ahead[-1], size, 2 * size, axis=axis)
    low = lax.ppermute(low, "sp", ring_pairs(n_sp, 1))
    high = lax.ppermute(high, "sp", ring_pairs(n_sp, -1))
    return behind, ahead, (low, high)


def vmem(n):
    return [pl.BlockSpec(memory_space=pltpu.VMEM)] * n


def per_device(
    skip_connection_stream,
    probing_vectors,
    addressing_vectors,
    mapped_payloads,
    emission_switch,
    lapse_preactivation,
    lapse_shift_entries,
    surplus_attenuation_terms,
    passage_label_per_token,
    attention_group_rescaler,
    emission_projector,
    perceptron_rescaler,
    switching_projector,
    widening_projector,
    shrinking_projector,
):
    rows_here, width = probing_vectors.shape
    heads = width // DK
    n_sp, n_tp = lax.axis_size("sp"), lax.axis_size("tp")
    place, group = lax.axis_index("sp"), lax.axis_index("tp")
    docs = passage_label_per_token

    def to_later(a, step):
        return lax.ppermute(a, "tp", [(i, (i + step) % n_tp) for i in range(n_tp)])

    both_w = jnp.concatenate([switching_projector, widening_projector], axis=1)
    both_first = ring_start(both_w, n_sp)
    down_first = ring_start(shrinking_projector, n_sp)
    projectors = [emission_projector] + [to_later(emission_projector, s) for s in range(1, n_tp)]

    local_out, qrun, state, total = pl.pallas_call(
        local_pass,
        out_shape=(
            jax.ShapeDtypeStruct((rows_here, heads * DV), F32),
            jax.ShapeDtypeStruct((rows_here, width), BF16),
            jax.ShapeDtypeStruct((width, DV), F32),
            jax.ShapeDtypeStruct((1, width), F32),
        ),
        in_specs=vmem(8),
        out_specs=tuple(vmem(4)),
        cost_estimate=pl.CostEstimate(
            flops=40_000_000_000, bytes_accessed=6_000_000, transcendentals=0
        ),
        name="local_pass",
    )(
        probing_vectors,
        addressing_vectors,
        mapped_payloads,
        lapse_preactivation,
        lapse_shift_entries[None, :],
        surplus_attenuation_terms[:, None],
        docs[:, None],
        docs.reshape(-1, BLOCK),
    )

    unbroken = (docs[0] == docs[-1]).astype(F32)
    ends = jnp.stack([docs[0], docs[-1]]).astype(BF16)
    small = jnp.concatenate([(jnp.exp(total[0]) * unbroken).astype(BF16), ends])
    tail_rows = 16 * pl.cdiv(small.size, 16 * DV)
    small = jnp.pad(small, (0, tail_rows * DV - small.size)).reshape(tail_rows, DV)
    packed = jnp.concatenate([state.astype(BF16), small], axis=0)
    half = (width + tail_rows) // 2
    first_half = lax.all_gather(packed[:half], "sp")
    packed, first_half, both_first = lax.optimization_barrier((packed, first_half, both_first))
    second_half = lax.all_gather(packed[half:], "sp")
    packed = jnp.concatenate([first_half, second_half], axis=1)
    behind, ahead, opposite = ring_rest(both_first, n_sp, 1)
    down_first, opposite = lax.optimization_barrier((down_first, opposite))
    down_behind, down_ahead, down_opposite = ring_rest(down_first, n_sp, 0)

    ring = jnp.asarray(ring_orders(n_sp), jnp.int32)
    count = n_sp // 2
    spot = jnp.argmax(ring == place // 2)
    core = place % 2

    def chip_at(steps_behind):
        return ring[(spot - steps_behind + count) % count]

    chips = [chip_at(0)]
    chips += [chip_at(d + 1) for d in range(len(behind))]
    chips += [chip_at(-d - 1) for d in range(len(ahead))]
    chips += [chip_at(count // 2)]
    owners = [2 * c + core for c in chips] + [2 * c + 1 - core for c in chips]
    lows, highs = opposite
    here = [both_w] + behind + ahead + [jnp.concatenate([lows, highs], axis=1)]
    there = [swap_cores(a, n_sp) for a in [both_w] + behind + ahead]
    there += [jnp.concatenate([swap_cores(lows, n_sp), swap_cores(highs, n_sp)], axis=1)]
    hidden_width = switching_projector.shape[1]
    gate_w = jnp.concatenate([a[:, :hidden_width] for a in here + there], axis=0)
    up_w = jnp.concatenate([a[:, hidden_width:] for a in here + there], axis=0)
    down_here = [shrinking_projector] + down_behind + down_ahead
    down_there = [swap_cores(a, n_sp) for a in down_here]
    states = packed[:, :width]
    smalls = packed[:, width:].reshape(n_sp, -1).astype(F32)
    decays, first_doc, last_doc = smalls[:, :width], smalls[:, width], smalls[:, width + 1]
    before = jnp.concatenate([jnp.full((1,), -1.0, F32), last_doc[:-1]])
    decays = decays * (before == first_doc).astype(F32)[:, None]
    entering = jnp.zeros((width, DV), F32)
    for j in range(n_sp):
        entering = jnp.where(
            j < place, entering * decays[j][:, None] + states[j].astype(F32), entering
        )
    reaches = (docs.astype(F32) == before[place]).astype(F32)

    gated = pl.pallas_call(
        finish_pass,
        out_shape=jax.ShapeDtypeStruct((rows_here, heads * DV), BF16),
        in_specs=vmem(6),
        out_specs=vmem(1)[0],
        cost_estimate=pl.CostEstimate(
            flops=5_000_000_000, bytes_accessed=5_000_000, transcendentals=0
        ),
        name="finish_pass",
    )(
        local_out,
        qrun,
        entering.astype(BF16),
        reaches[:, None],
        emission_switch,
        attention_group_rescaler[None, :],
    )

    gateds = [gated] + [to_later(gated, s) for s in range(1, n_tp)]
    mixed = jnp.zeros((), F32)
    for rows, weight in zip(gateds, projectors):
        part = jnp.dot(rows, weight, preferred_element_type=F32).astype(BF16)
        mixed = mixed + part.astype(F32)
    first_all = (skip_connection_stream.astype(F32) + mixed).astype(BF16)
    normed = rms_rows(first_all, perceptron_rescaler)
    block = switching_projector.shape[0]

    def columns(a, owner):
        return lax.dynamic_slice_in_dim(a, owner * block, block, 1)

    ringed = jnp.concatenate([columns(normed, owner) for owner in owners], axis=1)
    gate = jnp.dot(ringed, gate_w, preferred_element_type=F32)
    upper = jnp.dot(ringed, up_w, preferred_element_type=F32)
    hidden = (jax.nn.silu(gate) * upper).astype(BF16)

    share = rows_here // n_tp

    def share_of(a, owner):
        return lax.dynamic_slice_in_dim(a, owner * share, share, 0)

    def reduced(weight):
        def down(owner):
            return jnp.dot(share_of(hidden, owner), weight, preferred_element_type=F32).astype(BF16)

        arrived = [to_later(down((group + s) % n_tp), s) for s in range(1, n_tp)]
        total = down(group).astype(F32)
        for part in arrived:
            total = total + part.astype(F32)
        return total

    late_here = jnp.concatenate(down_opposite, axis=0)
    late_there = jnp.concatenate([swap_cores(a, n_sp) for a in down_opposite], axis=0)
    near = (len(down_here) + 1) // 2
    order = [0] + [i + 1 + j * len(down_behind) for i in range(len(down_behind)) for j in (0, 1)]
    groups = [order[:near], order[near:], [len(down_here)]]
    down_here, down_there = down_here + [late_here], down_there + [late_there]
    first_own = share_of(first_all, group)
    out = first_own
    for members in groups:
        weight = jnp.concatenate(
            [down_here[i] for i in members] + [down_there[i] for i in members], axis=1
        )
        whose = [owners[i] for i in members] + [owners[len(chips) + i] for i in members]
        total = reduced(weight)
        for i, owner in enumerate(whose):
            start = (0, owner * block)
            piece = total[:, i * block : (i + 1) * block]
            base = lax.dynamic_slice(first_own, start, (share, block)).astype(F32)
            out = lax.dynamic_update_slice(out, (base + 0.5 * piece).astype(BF16), start)
    return out


def solution(mesh):
    placed = (
        P("sp", None),
        P("sp", "tp"),
        P("sp", "tp"),
        P("sp", "tp"),
        P("sp", "tp"),
        P("sp", "tp"),
        P("tp"),
        P("sp"),
        P("sp"),
        P(),
        P("tp", None),
        P(),
        P("sp", "tp"),
        P("sp", "tp"),
        P("tp", "sp"),
    )
    return jax.shard_map(
        per_device, mesh=mesh, in_specs=placed, out_specs=P(("sp", "tp"), None), check_vma=False
    )
```
